32 devices in a mesh: rep: 2 (over x), fs: 4 (over z), tp: 4 (over y, core).
Axes of the slice: x: 2, y: 2, z: 4, core: 2. Of those that a mesh axis runs over, the one named last changes fastest.
Arguments:
- tokens: bfloat16 [6144, 2048], P(('rep', 'fs'), 'tp'), may hold values from -6 to 6
- gain_mix: bfloat16 [2048], replicated, may hold values from 0.099609375 to 1.8984375
- query_weight: bfloat16 [2048, 1024], P('fs', 'tp'), may hold values from -0.125 to 0.125
- key_weight: bfloat16 [2048, 1024], P('fs', 'tp'), may hold values from -0.125 to 0.125
- value_weight: bfloat16 [2048, 2048], P('fs', 'tp'), may hold values from -0.125 to 0.125
- gate_weight: bfloat16 [2048, 2048], P('fs', 'tp'), may hold values from -0.125 to 0.125
- decay_rate: float32 [8], P('tp'), may hold values from 0.0006510417 to 0.05
- out_weight: bfloat16 [2048, 2048], P('tp', 'fs'), may hold values from -0.125 to 0.125
- gain_mlp: bfloat16 [2048], replicated, may hold values from 0.099609375 to 1.8984375
- up_weight: bfloat16 [2048, 8192], P('fs', 'tp'), may hold values from -0.125 to 0.125
- down_weight: bfloat16 [8192, 2048], P('tp', 'fs'), may hold values from -0.0625 to 0.0625
Outputs:
- layer_out: bfloat16 [6144, 2048], P(('rep', 'fs'), 'tp')
The draws below stay inside these ranges and needn't reach their ends.
All inputs are finite; a program needn't handle non-finite values.
Results may differ from the reference program's by a relative error of at most 0.019.
Values may be sent and summed in bfloat16 or wider, within the bound.
No kernel may reach another device: no remote copies, remote signals or barrier semaphores. Data moves between devices by JAX's collectives and lax.ppermute only.
A program may use at most 128 MiB of HBM per device.

```python
import math
import jax
import jax.numpy as jnp
from jax import lax

D = 2048
HEADS = 8
DK = 128
DV = 256
FF = 8192
SEQ = 768
BLK = 128
TOKENS = 6144
N_TP = 4


def steps_of(rng, shape, pieces, low, top_value):
    level, own = 1.0, jax.random.fold_in(rng, 6)
    for dim, shards_of in pieces:
        heights = jnp.exp(jax.random.uniform(jax.random.fold_in(own, dim), (shards_of,), jnp.float32, low / len(pieces), top_value / len(pieces)))
        level = level * jnp.repeat(heights, shape[dim] // shards_of).reshape([-1 if axis == dim else 1 for axis in range(len(shape))])
    return level


def centred(own_key, dims, spread, bound, split=(), held_as=jnp.bfloat16):
    entries = spread * jax.random.normal(own_key, dims, jnp.float32)
    if split:
        entries = entries * steps_of(own_key, dims, split, -0.22, 0.18)
    return jnp.clip(entries, -bound, bound).astype(held_as)


def setup_inputs(seed: int = 0) -> dict:
    key_list = jax.random.split(jax.random.key(seed), 12)
    tokens = centred(key_list[0], (TOKENS, D), 1.0, 6.0, ((0, 8), (1, 4)))
    gain_mix = jnp.clip(1.0 + 0.18 * jax.random.normal(key_list[1], (D,), jnp.float32), 0.099609375, 1.8984375).astype(jnp.bfloat16)
    query_weight = centred(key_list[2], (D, HEADS * DK), D ** -0.5, 0.125, ((0, 4), (1, 4)))
    key_weight = centred(key_list[3], (D, HEADS * DK), D ** -0.5, 0.125, ((0, 4), (1, 4)))
    value_weight = centred(key_list[4], (D, HEADS * DV), D ** -0.5, 0.125, ((0, 4), (1, 4)))
    gate_weight = centred(key_list[5], (D, HEADS * DV), D ** -0.5, 0.125, ((0, 4), (1, 4)))
    decay_rate = jnp.clip(jnp.exp(math.log(0.05) - 4.3412046 * jax.random.uniform(key_list[6], (HEADS,), jnp.float32) ** steps_of(key_list[6], (HEADS,), ((0, 4),), -0.2, 0.2)), 0.0006510417, 0.05)
    out_weight = centred(key_list[7], (HEADS * DV, D), (HEADS * DV) ** -0.5, 0.125, ((0, 4), (1, 4)))
    gain_mlp = jnp.clip(1.0 + 0.18 * jax.random.normal(key_list[8], (D,), jnp.float32), 0.099609375, 1.8984375).astype(jnp.bfloat16)
    up_weight = centred(key_list[9], (D, FF), D ** -0.5, 0.125, ((0, 4), (1, 4)))
    down_weight = centred(key_list[10], (FF, D), FF ** -0.5, 0.0625, ((0, 4), (1, 4)))
    return dict(tokens=tokens, gain_mix=gain_mix, query_weight=query_weight, key_weight=key_weight, value_weight=value_weight, gate_weight=gate_weight, decay_rate=decay_rate, out_weight=out_weight, gain_mlp=gain_mlp, up_weight=up_weight, down_weight=down_weight)


epsilon = 1e-06
highest = lax.Precision.HIGHEST

def rms_rows(rows, gain):
    values = rows.astype(jnp.float32)
    scaled = values * lax.rsqrt(lax.optimization_barrier(jnp.mean(values * values, axis=-1, keepdims=True)) + epsilon)
    return (scaled * gain.astype(jnp.float32)).astype(jnp.bfloat16)

def retain(query, keys, values, rate, block):
    length, head_count, key_width = query.shape
    value_width = values.shape[-1]
    block_count = length // block
    log_decay = -rate.astype(jnp.float32)
    positions = jnp.arange(block, dtype=jnp.float32)
    distance = positions[:, None] - positions[None, :]
    causal = distance >= 0
    inside = jnp.where(causal[None], jnp.exp(log_decay[:, None, None] * jnp.where(causal, distance, 0.0)[None]), 0.0)
    key_scale = jnp.exp(log_decay[None, :] * (block - 1.0 - positions)[:, None])
    query_scale = jnp.exp(log_decay[None, :] * (positions + 1.0)[:, None])
    carry_decay = jnp.exp(log_decay * block)
    query_blocks = query.reshape(block_count, block, head_count, key_width)
    key_blocks = keys.reshape(block_count, block, head_count, key_width) * key_width ** (-0.5)
    value_blocks = values.reshape(block_count, block, head_count, value_width)

    def advance(state, blocks):
        q_block, k_block, v_block = blocks
        scores = jnp.einsum('ihd,jhd->hij', q_block, k_block, precision=highest) * inside
        inner = jnp.einsum('hij,jhe->ihe', scores, v_block, precision=highest)
        cross = jnp.einsum('ihd,hde->ihe', q_block, state, precision=highest) * query_scale[:, :, None]
        update = jnp.einsum('jhd,jhe->hde', k_block * key_scale[:, :, None], v_block, precision=highest)
        return (state * carry_decay[:, None, None] + update, inner + cross)
    initial = jnp.zeros((head_count, key_width, value_width), jnp.float32)
    _, results = lax.scan(advance, initial, (query_blocks, key_blocks, value_blocks))
    return results.reshape(length, head_count, value_width)

def gated_heads(retained, gate):
    length, head_count, value_width = retained.shape
    normed = retained * lax.rsqrt(lax.optimization_barrier(jnp.mean(retained * retained, axis=-1, keepdims=True)) + epsilon)
    gated = jax.nn.silu(gate.reshape(length, head_count, value_width)) * normed
    return gated.reshape(length, head_count * value_width).astype(jnp.bfloat16)

def grouped_sum(left, right, groups):
    rows = left.shape[0]
    inner_width = left.shape[1] // groups
    left_groups = left.reshape(rows, groups, inner_width).astype(jnp.float32)
    right_groups = right.reshape(groups, inner_width, right.shape[1]).astype(jnp.float32)
    parts = jnp.einsum('sgc,gcd->gsd', left_groups, right_groups)
    rounded = lax.optimization_barrier(parts.astype(jnp.bfloat16)).astype(jnp.float32)
    return lax.optimization_barrier(jnp.sum(rounded, axis=0))

def reference(tokens, gain_mix, query_weight, key_weight, value_weight, gate_weight, decay_rate, out_weight, gain_mlp, up_weight, down_weight):

    def one_sequence(rows):
        normed = rms_rows(rows, gain_mix)
        query = jnp.dot(normed, query_weight, preferred_element_type=jnp.float32).reshape(SEQ, HEADS, DK)
        keys = jnp.dot(normed, key_weight, preferred_element_type=jnp.float32).reshape(SEQ, HEADS, DK)
        values = jnp.dot(normed, value_weight, preferred_element_type=jnp.float32).reshape(SEQ, HEADS, DV)
        gate = jnp.dot(normed, gate_weight, preferred_element_type=jnp.float32)
        retained = retain(query, keys, values, decay_rate, BLK)
        hidden = gated_heads(retained, gate)
        mixed = (rows.astype(jnp.float32) + grouped_sum(hidden, out_weight, N_TP)).astype(jnp.bfloat16)
        normed_mlp = rms_rows(mixed, gain_mlp)
        upward = jnp.dot(normed_mlp, up_weight, preferred_element_type=jnp.float32)
        active = jnp.square(jax.nn.relu(upward)).astype(jnp.bfloat16)
        return (mixed.astype(jnp.float32) + grouped_sum(active, down_weight, N_TP)).astype(jnp.bfloat16)
    sequences = tokens.reshape(TOKENS // SEQ, SEQ, D)
    return lax.map(one_sequence, sequences).reshape(TOKENS, D)
```

```python
import jax
import jax.numpy as jnp
from jax import lax
from jax.sharding import PartitionSpec as P

DK = 128
DV = 256
BLK = 128


epsilon = 1e-06
highest = lax.Precision.HIGHEST


def rms_rows(rows, gain):
    values = rows.astype(jnp.float32)
    scaled = values * lax.rsqrt(jnp.mean(values * values, axis=-1, keepdims=True) + epsilon)
    return (scaled * gain.astype(jnp.float32)).astype(jnp.bfloat16)


def retain(query, keys, values, rate, block):
    length, head_count, key_width = query.shape
    value_width = values.shape[-1]
    block_count = length // block
    log_decay = -rate
    positions = jnp.arange(block, dtype=jnp.float32)
    distance = positions[:, None] - positions[None, :]
    causal = distance >= 0
    inside = jnp.where(
        causal[None],
        jnp.exp(log_decay[:, None, None] * jnp.where(causal, distance, 0.0)[None]),
        0.0,
    )
    key_scale = jnp.exp(log_decay[None, :] * (block - 1.0 - positions)[:, None])
    query_scale = jnp.exp(log_decay[None, :] * (positions + 1.0)[:, None])
    carry_decay = jnp.exp(log_decay * block)
    query_blocks = query.reshape(block_count, block, head_count, key_width)
    key_blocks = keys.reshape(block_count, block, head_count, key_width) * key_width ** (-0.5)
    value_blocks = values.reshape(block_count, block, head_count, value_width)

    def advance(state, blocks):
        q_block, k_block, v_block = blocks
        scores = jnp.einsum("ihd,jhd->hij", q_block, k_block, precision=highest) * inside
        inner = jnp.einsum("hij,jhe->ihe", scores, v_block, precision=highest)
        cross = (
            jnp.einsum("ihd,hde->ihe", q_block, state, precision=highest) * query_scale[:, :, None]
        )
        update = jnp.einsum(
            "jhd,jhe->hde", k_block * key_scale[:, :, None], v_block, precision=highest
        )
        return (state * carry_decay[:, None, None] + update, inner + cross)

    initial = jnp.zeros((head_count, key_width, value_width), jnp.float32)
    _, results = lax.scan(advance, initial, (query_blocks, key_blocks, value_blocks))
    return results.reshape(length, head_count, value_width)


def gated_heads(retained, gate):
    length, head_count, value_width = retained.shape
    normed = retained * lax.rsqrt(jnp.mean(retained * retained, axis=-1, keepdims=True) + epsilon)
    gated = jax.nn.silu(gate.reshape(length, head_count, value_width)) * normed
    return gated.reshape(length, head_count * value_width).astype(jnp.bfloat16)


def add_rows(left, piece):
    return jnp.dot(left, piece, preferred_element_type=jnp.float32)


def local(
    tokens,
    gain_mix,
    query_weight,
    key_weight,
    value_weight,
    gate_weight,
    decay_rate,
    out_weight,
    gain_mlp,
    up_weight,
    down_weight,
):
    length = tokens.shape[0]
    whole_rows = lax.all_gather(tokens, "tp", axis=1, tiled=True)
    normed = rms_rows(whole_rows, gain_mix)

    def add_pair(pieces):
        return (add_rows(normed, pieces[0]), add_rows(normed, pieces[1]))

    query, keys = add_pair(
        (
            lax.all_gather(query_weight, "fs", axis=0, tiled=True),
            lax.all_gather(key_weight, "fs", axis=0, tiled=True),
        )
    )
    values, gate = add_pair(
        (
            lax.all_gather(value_weight, "fs", axis=0, tiled=True),
            lax.all_gather(gate_weight, "fs", axis=0, tiled=True),
        )
    )
    head_local = decay_rate.shape[0]
    retained = retain(
        query.reshape(length, head_local, DK),
        keys.reshape(length, head_local, DK),
        values.reshape(length, head_local, DV),
        decay_rate,
        BLK,
    )
    hidden = gated_heads(retained, gate)
    mix_terms = jnp.dot(
        hidden,
        lax.all_gather(out_weight, "fs", axis=1, tiled=True),
        preferred_element_type=jnp.float32,
    )
    mix_share = lax.psum_scatter(
        mix_terms.astype(jnp.bfloat16), "tp", scatter_dimension=1, tiled=True
    ).astype(jnp.float32)
    mixed = (tokens.astype(jnp.float32) + mix_share).astype(jnp.bfloat16)
    mixed_rows = lax.all_gather(mixed, "tp", axis=1, tiled=True)
    normed_mlp = rms_rows(mixed_rows, gain_mlp)
    upward = add_rows(normed_mlp, lax.all_gather(up_weight, "fs", axis=0, tiled=True))
    active = jnp.square(jax.nn.relu(upward)).astype(jnp.bfloat16)
    mlp_terms = jnp.dot(
        active,
        lax.all_gather(down_weight, "fs", axis=1, tiled=True),
        preferred_element_type=jnp.float32,
    )
    mlp_share = lax.psum_scatter(
        mlp_terms.astype(jnp.bfloat16), "tp", scatter_dimension=1, tiled=True
    ).astype(jnp.float32)
    return (mixed.astype(jnp.float32) + mlp_share).astype(jnp.bfloat16)


def retain_whole(query, keys, values, rate):
    positions = jnp.arange(query.shape[0], dtype=jnp.float32)
    distance = positions[:, None] - positions[None, :]
    decay = jnp.where(
        distance >= 0, jnp.exp(-rate * jnp.maximum(distance, 0.0)) * DK ** (-0.5), 0.0
    )
    scores = lax.dot_general(
        query.astype(jnp.bfloat16),
        keys.astype(jnp.bfloat16),
        (((1,), (1,)), ((), ())),
        preferred_element_type=jnp.float32,
    )
    return add_rows((scores * decay).astype(jnp.bfloat16), values.astype(jnp.bfloat16))


def ring_local(
    tokens,
    gain_mix,
    query_weight,
    key_weight,
    value_weight,
    gate_weight,
    decay_rate,
    out_weight,
    gain_mlp,
    up_weight,
    down_weight,
):
    n_fs = lax.axis_size("fs")
    r, z, t = lax.axis_index("rep"), lax.axis_index("fs"), lax.axis_index("tp")
    ring = [(i, (i + 1) % n_fs) for i in range(n_fs)]
    width = tokens.shape[1]

    def part(array, axis, whose):
        half = array.shape[axis] // 2
        return lax.dynamic_slice_in_dim(array, whose * half, half, axis)

    def halves(array, axis):
        return jnp.split(array, 2, axis=axis)

    def swap_rep(array):
        return lax.ppermute(array, "rep", [(0, 1), (1, 0)])

    def swap_tp(array, bit):
        return lax.ppermute(array, "tp", [(i, i ^ bit) for i in range(4)])

    def gather_tp(array):
        across = swap_tp(array, 2)
        return [array, swap_tp(array, 1), across, swap_tp(across, 1)]

    def gain_of(gain):
        blocks = gain.reshape(-1, width)
        return jnp.concatenate(
            [lax.dynamic_index_in_dim(blocks, t ^ d, 0, keepdims=False) for d in range(4)]
        )

    def scatter_tp(parts):
        from_core = swap_tp(jnp.stack([parts[3], parts[1]]), 1).astype(jnp.float32)
        across = (parts[2].astype(jnp.float32) + from_core[0]).astype(jnp.bfloat16)
        here = parts[0].astype(jnp.float32) + from_core[1]
        return here + swap_tp(across, 2).astype(jnp.float32)

    def both(whose):
        qv = jnp.concatenate([part(query_weight, 1, whose), part(value_weight, 1, whose)], axis=1)
        kg = jnp.concatenate([part(key_weight, 1, whose), part(gate_weight, 1, whose)], axis=1)
        return [
            (qv, kg),
            halves(part(out_weight, 0, whose), 0),
            halves(part(up_weight, 1, whose), 1),
            halves(part(down_weight, 0, whose), 0),
        ]

    mine, other = both(r), both(1 - r)
    arrived = []

    def send(piece):
        if len(arrived) >= 2:
            piece, _ = lax.optimization_barrier((piece, arrived[-2]))
        got = lax.ppermute(piece, "fs", ring)
        arrived.append(got)
        return got

    gathered = []
    for own, rest in zip(mine, other):
        steps = [(*own, *rest)]
        pieces = list(own)
        for _ in range(n_fs - 1):
            pieces = [send(p) for p in pieces]
            steps.append((*pieces, *[swap_rep(p) for p in pieces]))
        gathered.append(steps)

    def slot(k):
        return jnp.bitwise_xor((z - k) % n_fs, t)

    def stacked_rows(steps):
        columns = sum(p.shape[1] for p in steps[0])
        buffer = jnp.zeros((n_fs * width, columns), jnp.bfloat16)
        for k, pieces in enumerate(steps):
            at = 0
            for p in pieces:
                buffer = lax.dynamic_update_slice(buffer, p, (slot(k) * width, at))
                at += p.shape[1]
        return buffer

    blocks = gather_tp(tokens)
    normed = rms_rows(jnp.concatenate(blocks, axis=1), gain_of(gain_mix))
    projected = add_rows(normed, stacked_rows(gathered[0]))
    hidden = []
    for h in range(2):
        q, v, k, g = jnp.split(
            projected[:, h * 2 * (DK + DV) : (h + 1) * 2 * (DK + DV)],
            [DK, DK + DV, 2 * DK + DV],
            axis=1,
        )
        rate = lax.dynamic_index_in_dim(decay_rate, r ^ h, 0, keepdims=False)
        hidden.append(gated_heads(retain_whole(q, k, v, rate)[:, None, :], g))
    hidden = jnp.concatenate(hidden, axis=1)

    def outward(left, steps):
        found = jnp.zeros((n_fs, left.shape[0], width), jnp.bfloat16)
        for k, pieces in enumerate(steps):
            term = add_rows(left, jnp.concatenate(pieces, axis=0)).astype(jnp.bfloat16)
            found = lax.dynamic_update_slice(found, term[None], (slot(k), 0, 0))
        return scatter_tp([found[d] for d in range(4)])

    mixed = (tokens.astype(jnp.float32) + outward(hidden, gathered[1])).astype(jnp.bfloat16)
    normed_mlp = rms_rows(jnp.concatenate(gather_tp(mixed), axis=1), gain_of(gain_mlp))
    upward = add_rows(normed_mlp, stacked_rows(gathered[2]))
    active = jnp.square(jax.nn.relu(upward)).astype(jnp.bfloat16)
    return (mixed.astype(jnp.float32) + outward(active, gathered[3])).astype(jnp.bfloat16)


def solution(mesh):
    sizes = mesh.shape
    ringed = sizes["rep"] == 2 and sizes["fs"] == 4 and sizes["tp"] == 4
    return jax.shard_map(
        ring_local if ringed else local,
        mesh=mesh,
        in_specs=(
            P(("rep", "fs"), "tp"),
            P(),
            P("fs", "tp"),
            P("fs", "tp"),
            P("fs", "tp"),
            P("fs", "tp"),
            P("tp"),
            P("tp", "fs"),
            P(),
            P("fs", "tp"),
            P("tp", "fs"),
        ),
        out_specs=P(("rep", "fs"), "tp"),
        check_vma=False,
    )
```
